32 devices in a mesh: ep: 8 (over z, x), tp: 4 (over y, core).
Axes of the slice: x: 2, y: 2, z: 4, core: 2. Of those that a mesh axis runs over, the one named last changes fastest.
Arguments:
- tokens: bfloat16 [1024, 2048], P('ep'), may hold values from -6 to 6
- routes: int32 [1024, 2], P('ep'), may hold values from 0 to 7, all different within a row; in each aligned block of 128 rows (0 to 127, 128 to 255, ...) at most 36 rows name the same one
- route_gates: float32 [1024, 2], P('ep'), may hold values from 0.1 to 2
- cotangent: bfloat16 [1024, 2048], P('ep'), may hold values from -40 to 40
- w_gate: bfloat16 [8, 2048, 1536], P('ep', None, 'tp'), may hold values from -0.125 to 0.125
- w_up: bfloat16 [8, 2048, 1536], P('ep', None, 'tp'), may hold values from -0.125 to 0.125
- w_down: bfloat16 [8, 1536, 2048], P('ep', 'tp'), may hold values from -0.15625 to 0.15625
- s_gate: bfloat16 [2048, 1536], P(None, 'tp'), may hold values from -0.125 to 0.125
- s_up: bfloat16 [2048, 1536], P(None, 'tp'), may hold values from -0.125 to 0.125
- s_down: bfloat16 [1536, 2048], P('tp'), may hold values from -0.15625 to 0.15625
Outputs:
- token_grad: bfloat16 [1024, 2048], P('ep', 'tp')
- gate_grad: float32 [1024, 2], P('ep')
- grad_gate: float32 [8, 2048, 1536], P('ep', None, 'tp')
- grad_up: float32 [8, 2048, 1536], P('ep', None, 'tp')
- grad_down: float32 [8, 1536, 2048], P('ep', 'tp')
- grad_shared: float32 [1536, 2048], P(('tp', 'ep'))
- norm_in: float32 [8, 2, 2048], P('ep')
- norm_down: float32 [8, 1536], P('ep', 'tp')
- norm_shared: float32 [1536], P(('tp', 'ep'))
The draws below stay inside these ranges and needn't reach their ends.
Inputs may be any that keep to these rules, and one draw needn't show every extreme that they name: `routes`: within the rows of one index of ep no expert is named by more than 36 assignments, a bound that some block reaches.
All inputs are finite; a program needn't handle non-finite values.
Results may differ from the reference program's by a relative error of at most 0.0095.
Values may be sent and summed in bfloat16 or wider, within the bound.
A program may use at most 64 MiB of HBM per device.

```python
import math
import jax
import jax.numpy as jnp
import numpy as np
from jax import lax

D = 2048
FF = 1536
SHARED = 1536
TOP_K = 2
TOK_DEV = 128
EXPERTS = 8
CAP = 36
ROWS = 288
TOKENS = 1024
N_EP = 8
N_TP = 4


def draw_cotangent(key, part):
    first = jax.random.fold_in(key, 11)
    second = jax.random.fold_in(key, 12)
    third = jax.random.fold_in(key, 13)
    values = jax.random.normal(first, (TOKENS, D), jnp.float32)
    column_scale = jnp.exp(jax.random.uniform(third, (1, D), jnp.float32, math.log(0.3), math.log(3.0)))
    row_scale = jnp.exp(jax.random.uniform(second, (TOKENS, 1), jnp.float32, math.log(0.3), math.log(3.0)))
    values = jnp.clip(values, -5.0, 5.0)
    return (0.3 * values * row_scale * column_scale).astype(jnp.bfloat16)


def shard_levels(own_key, dims, shards, least, largest):
    def one(dim, blocks):
        steps = jax.random.uniform(jax.random.fold_in(jax.random.fold_in(own_key, 6), dim), (blocks,), jnp.float32, least / len(shards), largest / len(shards))
        return jnp.repeat(jnp.exp(steps), dims[dim] // blocks).reshape((-1,) + (1,) * (len(dims) - dim - 1))

    gain = one(*shards[0])
    for cut in shards[1:]:
        gain = gain * one(*cut)
    return gain


def routed_block(rng, own, number, rows, amount, top, bound, slope):
    order = jax.random.permutation(rng, amount)
    crowded, ordinary = portions_of(amount, rows * top, bound, slope, True), portions_of(amount, rows * top, bound, slope, False)
    places = jnp.arange(amount)

    def named(sizes, turn):
        used = int((sizes > 0).sum())
        fixed = max(1, used // 4)
        shifted = fixed + (places - fixed + turn * (used - fixed)) % max(1, amount - fixed)
        return jnp.zeros((amount,), jnp.int32).at[order[jnp.where(places < fixed, places, shifted)]].set(jnp.asarray(sizes, jnp.int32))

    sizes = jnp.where(number % 4 == 0, named(crowded, number // 4), named(ordinary, number - number // 4 - 1))
    mixed = jax.random.permutation(jax.random.fold_in(own, 3), amount)
    donor, taker = mixed[0:amount // 2 * 2:2], mixed[1:amount // 2 * 2:2]
    slack = jnp.minimum(sizes[donor] - 1, bound - sizes[taker]) // 2
    slack = jnp.where((donor == order[0]) | (taker == order[0]) | (sizes[taker] == 0), 0, jnp.maximum(slack, 0))
    shifted = jax.random.randint(jax.random.fold_in(own, 4), (amount // 2,), 0, 1 << 20) % (slack + 1)
    sizes = sizes.at[donor].add(-shifted).at[taker].add(shifted)
    labels = jnp.searchsorted(jnp.cumsum(sizes), jnp.arange(rows * top), side="right").astype(jnp.int32)
    listing = labels.reshape(top, rows).T
    listing = listing[jax.random.permutation(jax.random.fold_in(own, 1), rows)]
    turn = jax.random.randint(jax.random.fold_in(own, 2), (rows, 1), 0, top)
    return jnp.take_along_axis(listing, (jnp.arange(top)[None, :] + turn) % top, axis=1)


def portions_of(number_of, total, reach, lean, full):
    portions = [(1 << 20) // math.isqrt(rank ** lean) + 1 for rank in range(1, number_of + 1)]
    largest = reach if full else min(reach, max(-(-total // number_of), total * portions[0] // sum(portions)))
    least = 1 if total - largest >= number_of - 1 else 0
    given, surplus = [largest] + [least] * (number_of - 1), total - largest - least * (number_of - 1)
    while surplus > 0:
        movable = [i for i in range(1, number_of) if given[i] < largest] or [i for i in range(1, number_of) if given[i] < reach]
        pool, budget = sum([portions[i] for i in movable]), surplus
        for i in movable:
            addition = min(reach - given[i], max(1, budget * portions[i] // pool), surplus)
            given[i] = given[i] + addition
            surplus = surplus - addition
    return np.array(given)


def centred(stream_key, shape, scale, bound, shards=(), kind=jnp.bfloat16):
    drawn = jax.random.normal(stream_key, shape, jnp.float32) * scale
    if len(shards) > 0:
        drawn = shard_levels(stream_key, shape, shards, -0.22, 0.18) * drawn
    return jnp.clip(drawn, min=-bound, max=bound).astype(kind)


def setup_inputs(seed: int = 0) -> dict:
    arg_keys = jax.random.split(jax.random.key(seed), 11)
    tokens = centred(arg_keys[0], (TOKENS, D), 1.0, 6.0, ((0, 8),))
    routes_keys = jax.random.split(jax.random.fold_in(arg_keys[1], 1), TOKENS // TOK_DEV)
    routes_turns = jax.random.permutation(jax.random.fold_in(arg_keys[1], 3), TOKENS // TOK_DEV)
    routes = jax.vmap(lambda own, number: routed_block(jax.random.fold_in(arg_keys[1], 2), own, number, TOK_DEV, EXPERTS, TOP_K, CAP, 1))(routes_keys, routes_turns).reshape((TOKENS, TOP_K))
    route_gates = jnp.clip(jnp.exp(math.log(2.0) - 2.9957323 * jax.random.uniform(arg_keys[2], (TOKENS, TOP_K), jnp.float32) ** shard_levels(arg_keys[2], (TOKENS, TOP_K), ((0, 8),), -0.2, 0.2)), 0.1, 2.0)
    cotangent = draw_cotangent(jax.random.fold_in(arg_keys[10], 71), 0)
    w_gate = centred(arg_keys[4], (EXPERTS, D, FF), D ** -0.5, 0.125, ((0, 8), (2, 4)))
    w_up = centred(arg_keys[5], (EXPERTS, D, FF), D ** -0.5, 0.125, ((0, 8), (2, 4)))
    w_down = centred(arg_keys[6], (EXPERTS, FF, D), FF ** -0.5, 0.15625, ((0, 8), (1, 4)))
    s_gate = centred(arg_keys[7], (D, SHARED), D ** -0.5, 0.125, ((1, 4),))
    s_up = centred(arg_keys[8], (D, SHARED), D ** -0.5, 0.125, ((1, 4),))
    s_down = centred(arg_keys[9], (SHARED, D), SHARED ** -0.5, 0.15625, ((0, 4),))
    return {"tokens": tokens, "routes": routes, "route_gates": route_gates, "cotangent": cotangent, "w_gate": w_gate, "w_up": w_up, "w_down": w_down, "s_gate": s_gate, "s_up": s_up, "s_down": s_down}


def slot_table(routes):
    chosen = routes.reshape(N_EP, TOK_DEV * TOP_K)
    expert_ids = jnp.arange(EXPERTS, dtype=jnp.int32)
    one_hot = (chosen[:, :, None] == expert_ids[None, None, :]).astype(jnp.int32)
    ranks = jnp.sum((jnp.cumsum(one_hot, axis=1) - one_hot) * one_hot, axis=2)
    source = jnp.arange(N_EP, dtype=jnp.int32)[:, None]
    slot_of = chosen * ROWS + source * CAP + ranks
    return slot_of.reshape(TOKENS * TOP_K).astype(jnp.int32)


def block_sum(d_gate, d_up, gate_weight, up_weight):
    block_width = gate_weight.shape[1] // N_TP
    running = jnp.zeros((d_gate.shape[0], gate_weight.shape[0]), jnp.float32)
    for block_index in range(N_TP):
        lower = block_index * block_width
        upper = lower + block_width
        block_term = jnp.dot(d_gate[:, lower:upper], gate_weight[:, lower:upper].T, preferred_element_type=jnp.float32)
        block_term = block_term + jnp.dot(d_up[:, lower:upper], up_weight[:, lower:upper].T, preferred_element_type=jnp.float32)
        rounded = lax.optimization_barrier(block_term.astype(jnp.bfloat16))
        running = running + rounded.astype(jnp.float32)
    return running


def swiglu_back(rows_x, rows_c, gate_weight, up_weight, down_weight):
    pre_gate = jnp.dot(rows_x, gate_weight, preferred_element_type=jnp.float32)
    pre_up = jnp.dot(rows_x, up_weight, preferred_element_type=jnp.float32)
    sigmoid_gate = jax.nn.sigmoid(pre_gate)
    activated = pre_gate * sigmoid_gate
    hidden = (activated * pre_up).astype(jnp.bfloat16)
    hidden_grad = jnp.dot(rows_c, down_weight.T, preferred_element_type=jnp.float32)
    d_gate = (hidden_grad * pre_up * sigmoid_gate * (1.0 + pre_gate * (1.0 - sigmoid_gate))).astype(jnp.bfloat16)
    d_up = (hidden_grad * activated).astype(jnp.bfloat16)
    return hidden, hidden_grad, d_gate, d_up


def expert_back(args):
    rows_x, rows_c, gate_weight, up_weight, down_weight = args
    hidden, hidden_grad, d_gate, d_up = swiglu_back(rows_x, rows_c, gate_weight, up_weight, down_weight)
    gate_dot = jnp.sum(hidden.astype(jnp.float32) * hidden_grad, axis=1).astype(jnp.bfloat16)
    grad_gate = jnp.dot(rows_x.T, d_gate, preferred_element_type=jnp.float32)
    grad_up = jnp.dot(rows_x.T, d_up, preferred_element_type=jnp.float32)
    grad_down = jnp.dot(hidden.T, rows_c, preferred_element_type=jnp.float32)
    slot_grad = block_sum(d_gate, d_up, gate_weight, up_weight)
    return grad_gate, grad_up, grad_down, slot_grad, gate_dot


def reference(tokens, routes, route_gates, cotangent, w_gate, w_up, w_down, s_gate, s_up, s_down):
    slot_of = slot_table(routes)
    token_of = (jnp.arange(TOKENS * TOP_K, dtype=jnp.int32) // TOP_K).astype(jnp.int32)
    row_token = jnp.full((EXPERTS * ROWS,), TOKENS, jnp.int32).at[slot_of].set(token_of)
    row_gate = jnp.zeros((EXPERTS * ROWS,), jnp.float32).at[slot_of].set(route_gates.reshape(TOKENS * TOP_K))
    padded_x = jnp.concatenate([tokens, jnp.zeros((1, D), jnp.bfloat16)], axis=0)
    padded_c = jnp.concatenate([cotangent, jnp.zeros((1, D), jnp.bfloat16)], axis=0)
    slot_x = padded_x[row_token].reshape(EXPERTS, ROWS, D)
    slot_c = (row_gate[:, None] * padded_c[row_token].astype(jnp.float32)).astype(jnp.bfloat16).reshape(EXPERTS, ROWS, D)
    grad_gate, grad_up, grad_down, slot_grad, gate_dot = lax.map(expert_back, (slot_x, slot_c, w_gate, w_up, w_down))
    routed = jax.ops.segment_sum(slot_grad.reshape(EXPERTS * ROWS, D), row_token, num_segments=TOKENS + 1)[:TOKENS]
    gate_grad = gate_dot.reshape(EXPERTS * ROWS)[slot_of].reshape(TOKENS, TOP_K).astype(jnp.float32) / route_gates
    s_hidden, s_hidden_grad, s_d_gate, s_d_up = swiglu_back(tokens, cotangent, s_gate, s_up, s_down)
    grad_shared = jnp.dot(s_hidden.T, cotangent, preferred_element_type=jnp.float32)
    shared_back = block_sum(s_d_gate, s_d_up, s_gate, s_up)
    token_grad = (shared_back + routed).astype(jnp.bfloat16)
    norm_in = jnp.stack([jnp.mean(grad_gate ** 2, axis=2), jnp.mean(grad_up ** 2, axis=2)], axis=1)
    norm_down = jnp.mean(grad_down ** 2, axis=2)
    norm_shared = jnp.mean(grad_shared ** 2, axis=1)
    return (token_grad, gate_grad, grad_gate, grad_up, grad_down, grad_shared, norm_in, norm_down, norm_shared)
```

```python
import functools

import jax
import jax.numpy as jnp
from jax import lax
from jax.experimental import pallas as pl
from jax.experimental.pallas import tpu as pltpu
from jax.sharding import PartitionSpec as P

MESH = pl.DeviceIdType.MESH
CORES = 2
LANES = 128
BF = jnp.bfloat16
F32 = jnp.float32


def dot(a, b, ca=1, cb=0):
    return lax.dot_general(a, b, (((ca,), (cb,)), ((), ())), preferred_element_type=F32)


def activations(pre_gate, pre_up, hidden_grad):
    sig = jax.nn.sigmoid(pre_gate)
    act = pre_gate * sig
    hidden = (act * pre_up).astype(BF)
    d_gate = (hidden_grad * pre_up * sig * (1.0 + pre_gate * (1.0 - sig))).astype(BF)
    d_up = (hidden_grad * act).astype(BF)
    return hidden, d_gate, d_up


def power_of_two(n):
    return n >= 4 and n & (n - 1) == 0


def flip(index, bits):
    place = 1
    while bits >= place:
        if bits & place:
            index = index + place * (1 - 2 * lax.rem(lax.div(index, place), 2))
        place *= 2
    return index


def onward_first(n):
    if n == 1:
        return [0]
    half = onward_first(n // 2)
    return [2 * r + 1 for r in half] + [2 * r for r in half]


def body(
    ep, tp, cap_pad, live,
    routes_h, gate_rows_h, tokens_h, cot_h, wg_h, wu_h, wd_h, sg_h, su_h, sd_h,
    token_out, gate_out, gg_out, gu_out, gd_out, shared_out, norm_in_out, norm_down_out, norm_sh_out,
    routes, gate_rows, tokens, cot, wg, wu, wd, sg, su, sd,
    send, rx, acc, hids, dgs, dus,
    term, half_rx, half_tx, pair, pair_rx,
    part_a, part_own, recv_a, part_b, recv_b, sh_a, sh_own, sh_recv_a, sh_b, sh_recv_b,
    back_tx, back_rx, gsend, gback, gtok, gtok_rx, sq, sq_rx,
    w_sem, d1_s, d1_r, d2_s, d2_r, pass_s, pass_r, ra_s, ra_r, rb_s, rb_r,
    bk_s, bk_r, g_s, g_r, gx_s, gx_r, q_s, q_r, sa_s, sa_r, sb_s, sb_r, h_s, h_r, rp_s, rp_r,
):
    me = lax.axis_index("ep")
    j = lax.axis_index("tp")
    core = lax.rem(j, CORES)
    y = lax.div(j, CORES)
    mate = j + 1 - 2 * core
    ny = tp // CORES
    rows = ep * cap_pad
    tok, width = tokens.shape
    share = width // tp
    top = routes.shape[0]
    ff = wg.shape[1]
    sr = shared_out.shape[0]
    paired = power_of_two(ep)
    batches = 2 if paired else 1
    h = ep // batches
    hrows = h * cap_pad
    filled = pl.ds(0, live)

    def to(m):
        return flip(me, m) if paired else lax.rem(me + m, ep)

    def source(m):
        return flip(me, m) if paired else lax.rem(me - m + ep, ep)

    def block_of(b):
        if batches == 1:
            return pl.ds(0, ep)
        return pl.ds(lax.div(flip(me, b * h), h) * h, h)

    barrier = pltpu.get_barrier_semaphore()
    for m in range(1, ep):
        pl.semaphore_signal(barrier, inc=1, device_id={"ep": to(m)}, device_id_type=MESH)
    for step in range(1, tp):
        pl.semaphore_signal(
            barrier, inc=1, device_id={"tp": lax.rem(j + step, tp)}, device_id_type=MESH
        )

    loads = [
        pltpu.make_async_copy(src, dst, w_sem.at[n])
        for n, (src, dst) in enumerate(
            [
                (routes_h, routes), (gate_rows_h, gate_rows), (tokens_h, tokens), (cot_h, cot),
                (sg_h, sg), (su_h, su), (sd_h, sd), (wg_h, wg), (wu_h, wu), (wd_h, wd),
            ]
        )
    ]
    for load in loads:
        load.start()

    started = []

    def remote(src, dst, ssem, rsem, **where):
        copy = pltpu.make_async_remote_copy(
            src_ref=src, dst_ref=dst, send_sem=ssem, recv_sem=rsem,
            device_id=where, device_id_type=MESH,
        )
        copy.start()
        return copy

    def sent(*args, **where):
        copy = remote(*args, **where)
        started.append(copy)
        return copy

    if live < cap_pad:
        rx[:, :, :, live:, :] = jnp.zeros((tp, 2, ep, cap_pad - live, share), BF)
        back_rx[:, live:, :] = jnp.zeros((ep, cap_pad - live, share), BF)

    sub = lax.broadcasted_iota(jnp.int32, (tok, tok), 0)
    lane = lax.broadcasted_iota(jnp.int32, (tok, tok), 1)

    def to_col(row):
        return jnp.sum(jnp.where(sub == lane, row, 0.0), axis=1, keepdims=True)

    def to_row(col, wide=None):
        n = col.shape[0]
        at = (n, wide or n)
        here = lax.broadcasted_iota(jnp.int32, at, 0) == lax.broadcasted_iota(jnp.int32, at, 1)
        return jnp.sum(jnp.where(here, col, 0.0), axis=0, keepdims=True)

    loads[0].wait()
    loads[1].wait()
    expert_row = [routes[k : k + 1, :].astype(F32) for k in range(top)]
    expert_col = [to_col(row) for row in expert_row]
    gate_col = [to_col(gate_rows[k : k + 1, :]) for k in range(top)]
    slot_row = []
    for k in range(top):
        slot = expert_row[k] * cap_pad
        for other in range(top):
            same = (expert_col[other] == expert_row[k]) & (sub < lane)
            slot = slot + jnp.sum(jnp.where(same, 1.0, 0.0), axis=0, keepdims=True)
        slot_row.append(slot)
    slot_col = [to_col(row) for row in slot_row]

    loads[2].wait()
    loads[3].wait()
    cols = pl.ds(pl.multiple_of(j * share, share), share)
    x_share = tokens[:, cols]
    c_share = cot[:, cols].astype(F32)
    slot_ids = lax.broadcasted_iota(jnp.int32, (rows, tok), 0).astype(F32)
    any_hot = jnp.zeros((rows, tok), F32)
    c_rows = jnp.zeros((rows, share), F32)
    for k in range(top):
        hot = jnp.where(slot_ids == slot_row[k], 1.0, 0.0)
        any_hot = any_hot + hot
        c_rows = c_rows + dot(hot.astype(BF), (gate_col[k] * c_share).astype(BF))
    x_rows = dot(any_hot.astype(BF), x_share)
    send[0] = x_rows.astype(BF).reshape(ep, cap_pad, share)
    send[1] = c_rows.astype(BF).reshape(ep, cap_pad, share)

    pl.semaphore_wait(barrier, ep + tp - 2)

    order = range(1, ep) if paired else sorted(range(1, ep), key=lambda m: -min(m, ep - m))
    d1 = {}
    for m in order:
        dest = to(m)
        d1[m] = sent(
            send.at[:, dest, filled], rx.at[j, :, me, filled], d1_s.at[m], d1_r.at[m], ep=dest
        )
    rx[j, :, me] = send[:, me]

    def forward(origin, b):
        block = rx.at[j, :, origin, filled]
        remote(block, block, d2_s.at[0], d2_r.at[j, b], tp=mate)
        for step in range(1, ny):
            other = lax.rem(y + step, ny) * CORES + core
            remote(block, block, d2_s.at[step], d2_r.at[j, b], tp=other)

    forward(me, 0)

    def pull(ms):
        for m in ms:
            d1[m].wait_recv()
            forward(source(m), m // h)

    def part_of(block, d_gate, d_up, gate_w, up_w):
        at = pl.ds(pl.multiple_of(block * share, share), share)
        return dot(d_gate, gate_w[at, :], 1, 1) + dot(d_up, up_w[at, :], 1, 1)

    far_y = [lax.rem(y + step, ny) for step in range(1, ny)] + [y]

    held, sa, halves, rs, rp = {}, [], {}, [], []

    def shared_act():
        loads[4].wait()
        gate = dot(tokens[...], sg[...])
        loads[5].wait()
        up = dot(tokens[...], su[...])
        loads[6].wait()
        held["act"] = activations(gate, up, dot(cot[...], sd[...], 1, 1))

    def shared_term():
        for chunk in range(tp):
            at = slice(chunk * share, (chunk + 1) * share)
            value = dot(held["act"][0], cot[:, at], 0, 0)
            for i in range(ep):
                term[i, :, at] = value[i * sr : (i + 1) * sr].astype(BF)
        if paired:
            for g in onward_first(ep // 2):
                halves[0, g] = sent(
                    term.at[flip(me, 2 * g + 1)], half_rx.at[g],
                    h_s.at[g], h_r.at[g], ep=flip(me, 1),
                )
        else:
            px = lax.rem(me, 2)
            for d in range(ep // 2):
                rs.append(
                    sent(
                        term.at[2 * d + 1 - px], half_rx.at[d], h_s.at[d], h_r.at[d],
                        ep=me + 1 - 2 * px,
                    )
                )

    def half_slot(stage):
        return ep - (ep >> stage)

    def half_sum(stage, r):
        value = term[flip(me, r << stage)].astype(F32)
        for q in range(stage):
            place = (r << stage) >> (q + 1)
            if (q, place) in halves:
                halves.pop((q, place)).wait_recv()
            value = value + half_rx[half_slot(q) + place].astype(F32)
        return value

    def half_step(stage, r):
        slot = half_slot(stage) + (r >> 1)
        half_tx[slot - ep // 2] = half_sum(stage, r).astype(BF)
        halves[stage, r >> 1] = sent(
            half_tx.at[slot - ep // 2], half_rx.at[slot], h_s.at[slot], h_r.at[slot],
            ep=flip(me, 1 << stage),
        )

    def pair_step():
        px = lax.rem(me, 2)
        group = lax.div(me, 2)
        groups = ep // 2
        for d in range(groups):
            rs[d].wait_recv()
        for step in range(groups):
            d = lax.rem(group + step, groups)
            pair[d] = (term[2 * d + px].astype(F32) + half_rx[d].astype(F32)).astype(BF)
            if step > 0:
                rp.append(
                    sent(
                        pair.at[d], pair_rx.at[group], rp_s.at[step], rp_r.at[step], ep=2 * d + px
                    )
                )
        pair_rx[group] = pair[group]

    def shared_parts():
        for n, yq in enumerate(far_y):
            sh_a[n] = part_of(yq * CORES + 1 - core, *held["act"][1:], sg, su).astype(BF)
            sa.append(sent(sh_a.at[n], sh_recv_a.at[n], sa_s.at[n], sa_r.at[n], tp=mate))

    def shared_own():
        for n, yq in enumerate(far_y):
            sh_own[n] = part_of(yq * CORES + core, *held["act"][1:], sg, su)

    sb = []

    def shared_cross():
        for n, yq in enumerate(far_y[:-1]):
            sa[n].wait_recv()
            sh_b[n] = (sh_own[n] + sh_recv_a[n].astype(F32)).astype(BF)
            sb.append(
                sent(sh_b.at[n], sh_recv_b.at[n], sb_s.at[n], sb_r.at[n], tp=yq * CORES + core)
            )

    def add_share(t, b, first=False):
        at = pl.ds(pl.multiple_of(t * share, share), share)
        blk = block_of(b)
        x_in = rx[t, 0, blk].reshape(hrows, share)
        c_in = rx[t, 1, blk].reshape(hrows, share)
        for n, value in enumerate(
            [dot(x_in, wg[at, :]), dot(x_in, wu[at, :]), dot(c_in, wd[:, at], 1, 1)]
        ):
            value = value.reshape(h, cap_pad, ff)
            acc[n, blk] = value if first else acc[n, blk] + value

    def arrived(t, b):
        block = rx.at[t, :, block_of(b), filled]
        pltpu.make_async_remote_copy(
            src_ref=block, dst_ref=block, send_sem=d2_s.at[0], recv_sem=d2_r.at[t, b],
            device_id={"tp": mate}, device_id_type=MESH,
        ).wait_recv()

    passed = {}

    def gather_near(b):
        add_share(j, b, True)
        arrived(mate, b)
        add_share(mate, b)

    def gather_cross(b):
        for step in range(1, ny):
            t = lax.rem(y - step + ny, ny) * CORES + core
            arrived(t, b)
            block = rx.at[t, :, block_of(b), filled]
            passed[step, b] = sent(block, block, pass_s.at[step, b], pass_r.at[step, b], tp=mate)
            add_share(t, b)

    def gather_last(b):
        for step in range(1, ny):
            passed[step, b].wait_recv()
            add_share(lax.rem(y - step + ny, ny) * CORES + 1 - core, b)

    grads, gs = {}, []

    def activate(b):
        blk = block_of(b)
        parts = [acc[n, blk].reshape(hrows, ff) for n in range(3)]
        hidden, d_gate, d_up = activations(*parts)
        hids[blk] = hidden.reshape(h, cap_pad, ff)
        dgs[blk] = d_gate.reshape(h, cap_pad, ff)
        dus[blk] = d_up.reshape(h, cap_pad, ff)
        grads[b] = d_gate, d_up
        dots = jnp.sum(hidden.astype(F32) * parts[2], axis=1, keepdims=True)
        for s in range(h):
            gsend[blk.start + s] = to_row(dots[s * cap_pad : (s + 1) * cap_pad], LANES)
        for m in range(b * h, (b + 1) * h):
            if m == 0:
                gback[me] = gsend[me]
            else:
                dest = to(m)
                gs.append(sent(gsend.at[dest], gback.at[me], g_s.at[m], g_r.at[m], ep=dest))

    ra, rb = {}, {}

    def parts_mate(b):
        blk = block_of(b)
        for n, yq in enumerate(far_y):
            value = part_of(yq * CORES + 1 - core, *grads[b], wg, wu).astype(BF)
            part_a[n, blk] = value.reshape(h, cap_pad, share)
            ra[n, b] = sent(
                part_a.at[n, blk, filled], recv_a.at[n, blk, filled],
                ra_s.at[n, b], ra_r.at[n, b], tp=mate,
            )

    def parts_own(b):
        blk = block_of(b)
        for n, yq in enumerate(far_y):
            value = part_of(yq * CORES + core, *grads[b], wg, wu)
            part_own[n, blk] = value.reshape(h, cap_pad, share)

    def back_order(b):
        return list(range((b + 1) * h - 1, b * h - 1, -1))

    def cross(b):
        for n in range(ny - 1):
            ra[n, b].wait_recv()
        for m in back_order(b):
            dest = to(m)
            for n in range(ny - 1):
                part_b[n, dest, :live] = (
                    part_own[n, dest, :live] + recv_a[n, dest, :live].astype(F32)
                ).astype(BF)
                rb[n, m] = sent(
                    part_b.at[n, dest, filled], recv_b.at[n, dest, filled],
                    rb_s.at[n, m], rb_r.at[n, m], tp=far_y[n] * CORES + core,
                )

    bk = []

    def back(m):
        b = m // h
        dest = to(m)
        if (ny - 1, b) in ra:
            ra.pop((ny - 1, b)).wait_recv()
        part = part_own[ny - 1, dest, :live] + recv_a[ny - 1, dest, :live].astype(F32)
        for n in range(ny - 1):
            rb[n, m].wait_recv()
            part = part + recv_b[n, dest, :live].astype(F32)
        if m == 0:
            back_rx[me, :live] = part.astype(BF)
        else:
            back_tx[dest, :live] = part.astype(BF)
            bk.append(
                sent(
                    back_tx.at[dest, filled], back_rx.at[me, filled],
                    bk_s.at[m], bk_r.at[m], ep=dest,
                )
            )

    down = []

    def weight_grads(t):
        at = slice(t * share, (t + 1) * share)
        x_in = rx[t, 0].reshape(rows, share)
        c_in = rx[t, 1].reshape(rows, share)
        for n, (out, grad) in enumerate([(gg_out, dgs), (gu_out, dus)]):
            value = dot(x_in, grad[...].reshape(rows, ff), 0, 0)
            out[at, :] = value
            col = jnp.sum(jnp.square(value), axis=1, keepdims=True)
            for i in range(share // LANES):
                lanes = slice(t * share + i * LANES, t * share + (i + 1) * LANES)
                sq[n : n + 1, lanes] = to_row(col[i * LANES : (i + 1) * LANES])
        value = dot(hids[...].reshape(rows, ff), c_in, 0, 0)
        gd_out[:, at] = value
        down.append(jnp.sum(jnp.square(value), axis=1, keepdims=True))

    near, far = list(order)[: h - 1], list(order)[h - 1 :]
    last = batches - 1

    shared_act()
    shared_term()
    pull(near[:1])
    shared_parts()
    pull(near[1:])
    for load in loads[7:]:
        load.wait()
    shared_own()
    if batches > 1:
        gather_near(0)
        pull(far[:1])
        gather_cross(0)
        pull(far[1:2])
        gather_last(0)
        activate(0)
        pull(far[2:3])
        parts_mate(0)
        half_step(1, 3) if ep == 8 else None
        pull(far[3:])
        parts_own(0)
        cross(0)
    gather_near(last)
    gather_cross(last)
    gather_last(last)
    activate(last)
    parts_mate(last)
    parts_own(last)
    cross(last)
    shared_cross()
    if batches > 1:
        for m in back_order(0):
            back(m)
    if paired:
        stage = 1
        while (1 << stage) < ep:
            for r in onward_first(ep >> stage):
                if r % 2 and (stage, r >> 1) not in halves:
                    half_step(stage, r)
            stage += 1
    else:
        pair_step()

    weight_grads(0)
    for m in back_order(last):
        back(m)
    for t in range(1, tp):
        weight_grads(t)
    norm_down_out[...] = to_row(functools.reduce(lambda a, b: a + b, down)) / width
    qx = [
        sent(sq, sq_rx.at[step], q_s.at[step], q_r.at[step], tp=lax.rem(j + step, tp))
        for step in range(1, tp)
    ]

    for copy in gs:
        copy.wait_recv()
    spot = lax.broadcasted_iota(jnp.int32, (tok, LANES), 1)
    spot_f = spot.astype(F32)
    for k in range(top):
        picked = jnp.zeros((tok, LANES), F32)
        for i in range(ep):
            hit = (spot < cap_pad) & (slot_col[k] == spot_f + float(i * cap_pad))
            picked = picked + jnp.where(hit, gback[i], 0.0)
        gtok[k : k + 1, :] = to_row(jnp.sum(picked, axis=1, keepdims=True))
    gx = [
        sent(gtok, gtok_rx.at[step], gx_s.at[step], gx_r.at[step], tp=lax.rem(j + step, tp))
        for step in range(1, tp)
    ]

    if paired:
        stage = 0
        while (1 << stage) < ep:
            stage += 1
        grad = half_sum(stage, 0)
    else:
        for copy in rp:
            copy.wait_recv()
        grad = pair_rx[0].astype(F32)
        for i in range(1, ep // 2):
            grad = grad + pair_rx[i].astype(F32)
    shared_out[...] = grad
    norm_sh_out[...] = to_row(jnp.mean(jnp.square(grad), axis=1, keepdims=True))

    for copy in qx:
        copy.wait_recv()
    squares = sq[...]
    for step in range(1, tp):
        squares = squares + sq_rx[step]
    norm_in_out[...] = squares / (tp * ff)

    for copy in gx:
        copy.wait_recv()
    dots = gtok[...]
    for step in range(1, tp):
        dots = dots + gtok_rx[step]
    gate_out[...] = dots.astype(BF).astype(F32) / gate_rows[...]

    sa[ny - 1].wait_recv()
    shared_tot = sh_own[ny - 1] + sh_recv_a[ny - 1].astype(F32)
    for n in range(ny - 1):
        sb[n].wait_recv()
        shared_tot = shared_tot + sh_recv_b[n].astype(F32)
    place = lax.broadcasted_iota(jnp.int32, (tok, rows), 1).astype(F32)
    pick = jnp.zeros((tok, rows), F32)
    for k in range(top):
        pick = pick + jnp.where(place == slot_col[k], 1.0, 0.0)
    for copy in bk:
        copy.wait_recv()
    token_out[...] = (
        dot(pick.astype(BF), back_rx[...].reshape(rows, share)) + shared_tot
    ).astype(BF)

    forwarded = rx.at[j, :, :, filled]
    for step in range(ny):
        pltpu.make_async_remote_copy(
            src_ref=forwarded, dst_ref=forwarded, send_sem=d2_s.at[step], recv_sem=d2_r.at[j, 0],
            device_id={"tp": mate}, device_id_type=MESH,
        ).wait_send()
    for copy in started:
        copy.wait_send()


def place_out(*refs):
    count = len(refs) // 2
    sem = refs[-1]
    copies = [
        pltpu.make_async_copy(refs[n], refs[count + n], sem.at[n]) for n in range(count)
    ]
    for copy in copies:
        copy.start()
    for copy in copies:
        copy.wait()


def on_device(
    ep, tp, tokens, routes, route_gates, cotangent, w_gate, w_up, w_down, s_gate, s_up, s_down
):
    tok, width = tokens.shape
    top = routes.shape[1]
    cap = max(2, (9 * tok * top + 8 * ep - 1) // (8 * ep))
    cap_pad = -(-cap // 16) * 16
    rows, share, ff, ny = ep * cap_pad, width // tp, w_gate.shape[2], tp // CORES
    sff = s_gate.shape[1]
    sr = sff // ep
    live = -(-cap // 8) * 8
    nb = 2 if power_of_two(ep) else 1
    groups = ep // 2

    vm, hbm = pl.BlockSpec(memory_space=pltpu.VMEM), pl.BlockSpec(memory_space=pl.ANY)
    dma = pltpu.SemaphoreType.DMA
    outs = [
        ((tok, share), BF), ((top, tok), F32), ((width, ff), F32), ((width, ff), F32),
        ((ff, width), F32), ((sr, width), F32), ((2, width), F32), ((1, ff), F32), ((1, sr), F32),
    ]
    slots = (ny, ep, cap_pad, share)
    spare = (1, 16, LANES)
    scratch = [
        pltpu.VMEM((top, tok), jnp.int32), pltpu.VMEM((top, tok), F32),
        pltpu.VMEM((tok, width), BF), pltpu.VMEM((tok, width), BF),
        pltpu.VMEM((width, ff), BF), pltpu.VMEM((width, ff), BF), pltpu.VMEM((ff, width), BF),
        pltpu.VMEM((width, sff), BF), pltpu.VMEM((width, sff), BF), pltpu.VMEM((sff, width), BF),
        pltpu.VMEM((2, ep, cap_pad, share), BF),
        pltpu.VMEM((tp, 2, ep, cap_pad, share), BF),
        pltpu.VMEM((3, ep, cap_pad, ff), F32),
        pltpu.VMEM((ep, cap_pad, ff), BF), pltpu.VMEM((ep, cap_pad, ff), BF),
        pltpu.VMEM((ep, cap_pad, ff), BF),
        pltpu.VMEM((ep, sr, width), BF),
        pltpu.VMEM((ep if nb > 1 else groups, sr, width), BF),
        pltpu.VMEM((groups, sr, width) if nb > 1 else spare, BF),
        pltpu.VMEM(spare if nb > 1 else (groups, sr, width), BF),
        pltpu.VMEM(spare if nb > 1 else (groups, sr, width), BF),
        pltpu.VMEM(slots, BF), pltpu.VMEM(slots, F32), pltpu.VMEM(slots, BF),
        pltpu.VMEM(slots, BF), pltpu.VMEM(slots, BF),
        pltpu.VMEM((ny, tok, share), BF), pltpu.VMEM((ny, tok, share), F32),
        pltpu.VMEM((ny, tok, share), BF), pltpu.VMEM((ny, tok, share), BF),
        pltpu.VMEM((ny, tok, share), BF),
        pltpu.VMEM((ep, cap_pad, share), BF), pltpu.VMEM((ep, cap_pad, share), BF),
        pltpu.VMEM((ep, 1, LANES), F32), pltpu.VMEM((ep, 1, LANES), F32),
        pltpu.VMEM((top, tok), F32), pltpu.VMEM((tp, top, tok), F32),
        pltpu.VMEM((2, width), F32), pltpu.VMEM((tp, 2, width), F32),
        dma((10,)), dma((ep,)), dma((ep,)), dma((ny,)), dma((tp, nb)),
        dma((ny, nb)), dma((ny, nb)), dma((ny, nb)), dma((ny, nb)), dma((ny, ep)), dma((ny, ep)),
        dma((ep,)), dma((ep,)), dma((ep,)), dma((ep,)), dma((tp,)), dma((tp,)), dma((tp,)), dma((tp,)),
        dma((ny,)), dma((ny,)), dma((ny,)), dma((ny,)), dma((ep,)), dma((ep,)), dma((ep,)), dma((ep,)),
    ]
    done = pl.pallas_call(
        functools.partial(body, ep, tp, cap_pad, live),
        out_shape=[pltpu.VMEM(shape, kind) for shape, kind in outs],
        in_specs=[hbm] * 10,
        out_specs=[vm] * 9,
        scratch_shapes=scratch,
        compiler_params=pltpu.CompilerParams(
            collective_id=0, has_side_effects=True, vmem_limit_bytes=48 * 1024 * 1024
        ),
    )(
        routes.T, route_gates.T, tokens, cotangent,
        w_gate[0], w_up[0], w_down[0], s_gate, s_up, s_down,
    )
    out = pl.pallas_call(
        place_out,
        out_shape=[jax.ShapeDtypeStruct(shape, kind) for shape, kind in outs],
        in_specs=[vm] * 9,
        out_specs=[hbm] * 9,
        scratch_shapes=[dma((9,))],
        compiler_params=pltpu.CompilerParams(vmem_limit_bytes=8 * 1024 * 1024),
    )(*[pltpu.with_memory_space_constraint(value, pltpu.VMEM) for value in done])
    token_grad, gate_grad, gg, gu, gd, grad_shared, norm_in, norm_down, norm_sh = out
    return (
        token_grad, gate_grad.T, gg[None], gu[None], gd[None], grad_shared, norm_in[None],
        norm_down.reshape(1, ff), norm_sh.reshape(sr),
    )


def solution(mesh):
    placed = (
        P("ep", None), P("ep", None), P("ep", None), P("ep", None),
        P("ep", None, "tp"), P("ep", None, "tp"), P("ep", "tp", None),
        P(None, "tp"), P(None, "tp"), P("tp", None),
    )
    return jax.shard_map(
        functools.partial(on_device, mesh.shape["ep"], mesh.shape["tp"]),
        mesh=mesh,
        in_specs=placed,
        out_specs=(
            P("ep", "tp"), P("ep", None), P("ep", None, "tp"), P("ep", None, "tp"),
            P("ep", "tp", None), P(("tp", "ep"), None), P("ep", None, None), P("ep", "tp"),
            P(("tp", "ep")),
        ),
        check_vma=False,
    )
```
